32 devices in a mesh: dp: 4 (over y, x), kv: 4 (over z), tp: 2 (over core).
Axes of the slice: x: 2, y: 2, z: 4, core: 2. Of those that a mesh axis runs over, the one named last changes fastest.
Arguments:
- tokens: bfloat16 [16, 4096], P('dp', ('kv', 'tp')), may hold values from -11 to 11
- attn_gain: float32 [4096], replicated, may hold values from 0.1 to 1.9
- query_weight: bfloat16 [4096, 4096], P('kv', 'tp'), may hold values from -0.09375 to 0.09375
- key_cache: bfloat16 [16, 1024, 2, 128], P('dp', 'kv', 'tp'), may hold values from -820 to 820
- value_cache: bfloat16 [16, 1024, 2, 128], P('dp', 'kv', 'tp'), may hold values from -6 to 6
- head_lambda: float32 [32], P('tp'), may hold values from 0.3 to 0.8
- head_gain: float32 [128], replicated, may hold values from 0.1 to 1.9
- out_weight: bfloat16 [4096, 4096], P('kv', 'tp'), may hold values from -0.09375 to 0.09375
- mlp_gain: float32 [4096], replicated, may hold values from 0.1 to 1.9
- gate_weight: bfloat16 [11264, 4096], P(('kv', 'tp')), may hold values from -0.09375 to 0.09375
- up_weight: bfloat16 [11264, 4096], P(('kv', 'tp')), may hold values from -0.09375 to 0.09375
- down_weight: bfloat16 [11264, 4096], P(('kv', 'tp')), may hold values from -0.078125 to 0.078125
Outputs:
- mixed: bfloat16 [16, 4096], P('dp', ('kv', 'tp'))
The draws below stay inside these ranges and needn't reach their ends.
All inputs are finite; a program needn't handle non-finite values.
Results may differ from the reference program's by a relative error of at most 0.02.
The reference program's roundings to bfloat16 on the way (of `scaled`, `rotated`, `probs`, `head_out`, `normed` and `hidden`) count: a program that leaves them out, or rounds other values in their place, can miss the bound.
Values may be sent and summed in bfloat16 or wider, within the bound.
A program may use at most 128 MiB of HBM per device.

```python
import jax
import jax.numpy as jnp
from jax import lax

D = 4096
HEADS = 32
KV_HEADS = 2
HEAD = 64
FF = 11264
VALUE = 128
GROUP = 16
BATCH = 16
CACHE_LEN = 1024
N_TP = 2


def draw_tokens(key, part):
    column_scale = 10.0 ** (jnp.arange(D, dtype=jnp.float32) / D - 0.5)
    row_scale = 10.0 ** (jax.random.uniform(jax.random.fold_in(key, 21), (BATCH, 1), jnp.float32) - 0.5)
    base = jnp.clip(jax.random.normal(jax.random.fold_in(key, 24), (BATCH, D), jnp.float32), -4.0, 4.0)
    return (0.25 * row_scale * column_scale * base).astype(jnp.bfloat16)


def draw_key_cache(key, part):
    shape = (BATCH, CACHE_LEN, KV_HEADS, 2 * HEAD)
    base = jnp.clip(jax.random.normal(jax.random.fold_in(key, 11), shape, jnp.float32), -4.0, 4.0)
    spots = jax.random.randint(jax.random.fold_in(key, 12), (BATCH, 1, KV_HEADS, 4), 0, CACHE_LEN - 1)
    strength = jax.random.uniform(jax.random.fold_in(key, 13), (BATCH, 1, KV_HEADS, 4), jnp.float32, 100.0, 200.0)
    flips = jax.random.randint(jax.random.fold_in(key, 14), (BATCH, 1, KV_HEADS, 4), 0, 2)
    signed = strength * (2.0 * flips.astype(jnp.float32) - 1.0)
    place = jnp.arange(CACHE_LEN, dtype=jnp.int32).reshape(1, CACHE_LEN, 1, 1)
    hits = place == spots
    factor = jnp.sum(jnp.where(hits, signed, 0.0), axis=-1, keepdims=True)
    marked = jnp.any(hits, axis=-1, keepdims=True)
    follow_factor = jnp.roll(factor, 1, axis=1)
    follow = jnp.logical_and(jnp.roll(marked, 1, axis=1), jnp.logical_not(marked))
    lifted = jnp.roll(base, 1, axis=1)
    planted = jnp.where(marked, factor * base, jnp.where(follow, 1.01 * follow_factor * lifted, 2.0 * base))
    return planted.astype(jnp.bfloat16)


def spiked(array, stream_key, source, target, blocks, factor):
    def block_of(dim):
        return (jnp.arange(array.shape[dim]) // (array.shape[dim] // blocks)).reshape((-1,) + (1,) * (array.ndim - 1 - dim))

    one_side = jax.random.permutation(stream_key, blocks)[block_of(target)]
    second = (block_of(target) + blocks // 2) % blocks
    return jnp.where((block_of(source) == one_side) | (block_of(source) == second), factor * array, array)


def levels(stream_key, dims, split, least, high):
    loudness, own = 1.0, jax.random.fold_in(stream_key, 6)
    for axis_at, blocks in split:
        steps = jnp.exp(jax.random.uniform(jax.random.fold_in(own, axis_at), (blocks,), jnp.float32, least / len(split), high / len(split)))
        loudness = loudness * jnp.repeat(steps, dims[axis_at] // blocks).reshape([-1 if axis == axis_at else 1 for axis in range(len(dims))])
    return loudness


def gaussian(own_key, dims, scale, most, cuts=(), kind=jnp.bfloat16):
    result = scale * jax.random.normal(own_key, dims, jnp.float32)
    if cuts:
        result = result * levels(own_key, dims, cuts, -0.22, 0.18)
    return jnp.clip(result, -most, most).astype(kind)


def gaussian_with(stream_key, dims, deviation, limit, pieces, heavy, kind=jnp.bfloat16):
    values = deviation * jax.random.normal(stream_key, dims, jnp.float32)
    if pieces:
        values = values * levels(stream_key, dims, pieces, -0.22, 0.18)
    return jnp.clip(spiked(values, jax.random.fold_in(stream_key, 3), *heavy), -limit, limit).astype(kind)


def setup_inputs(seed: int = 0) -> dict:
    key_of = jax.random.split(jax.random.key(seed), 13)
    return {
        "tokens": draw_tokens(jax.random.fold_in(key_of[12], 71), 0),
        "attn_gain": jnp.clip(1.0 + 0.18 * jax.random.normal(key_of[1], (D,), jnp.float32), 0.1, 1.9),
        "query_weight": gaussian(key_of[2], (D, HEADS * 2 * HEAD), D ** -0.5, 0.09375, ((0, 4), (1, 2))),
        "key_cache": draw_key_cache(jax.random.fold_in(key_of[12], 71), 0),
        "value_cache": gaussian(key_of[4], (BATCH, CACHE_LEN, KV_HEADS, VALUE), 1.0, 6.0, ((0, 4), (1, 4), (2, 2))),
        "head_lambda": jnp.clip(0.3 + 0.5 * jax.random.uniform(key_of[5], (HEADS,), jnp.float32) ** levels(key_of[5], (HEADS,), ((0, 2),), -0.2, 0.2), 0.3, 0.8),
        "head_gain": jnp.clip(1.0 + 0.18 * jax.random.normal(key_of[6], (VALUE,), jnp.float32), 0.1, 1.9),
        "out_weight": gaussian(key_of[7], (D, HEADS * VALUE), (HEADS * VALUE) ** -0.5, 0.09375, ((0, 4), (1, 2))),
        "mlp_gain": jnp.clip(1.0 + 0.18 * jax.random.normal(key_of[8], (D,), jnp.float32), 0.1, 1.9),
        "gate_weight": gaussian(key_of[9], (FF, D), D ** -0.5, 0.09375, ((0, 8),)),
        "up_weight": gaussian(key_of[10], (FF, D), D ** -0.5, 0.09375, ((0, 8),)),
        "down_weight": gaussian_with(key_of[11], (FF, D), FF ** -0.5, 0.078125, ((0, 8),), (0, 1, 8, 2.0)),
    }


EPS = 1e-06
THETA = 10000.0

def rotate(vector, position):
    half_len = vector.shape[-1] // 2
    inv_freq = 1.0 / THETA ** (jnp.arange(half_len, dtype=jnp.float32) / half_len)
    angles = position * inv_freq
    cos_table = jnp.cos(angles)
    sin_table = jnp.sin(angles)
    first_half = vector[..., :half_len]
    second_half = vector[..., half_len:]
    return jnp.concatenate([first_half * cos_table - second_half * sin_table, second_half * cos_table + first_half * sin_table], axis=-1)

def reference(tokens, attn_gain, query_weight, key_cache, value_cache, head_lambda, head_gain, out_weight, mlp_gain, gate_weight, up_weight, down_weight):
    as_float = tokens.astype(jnp.float32)
    mean_square = lax.optimization_barrier(jnp.mean(as_float * as_float, axis=-1, keepdims=True))
    scaled = (as_float * attn_gain).astype(jnp.bfloat16)
    queries = jnp.dot(scaled, query_weight, preferred_element_type=jnp.float32) * lax.rsqrt(mean_square + EPS)
    queries = queries.reshape(BATCH, HEADS, 2, HEAD)
    rotated = rotate(queries, jnp.float32(CACHE_LEN)).astype(jnp.bfloat16)
    lam_grid = head_lambda.reshape(KV_HEADS, GROUP, 1)

    def attend(item):
        query_row, key_rows, value_rows = item
        query_grid = query_row.reshape(KV_HEADS, GROUP, 2, HEAD).astype(jnp.float32)
        key_grid = key_rows.reshape(CACHE_LEN, KV_HEADS, 2, HEAD).astype(jnp.float32)
        scores = jnp.einsum('kgch,lkch->kgcl', query_grid, key_grid) * HEAD ** (-0.5)
        top_score = lax.optimization_barrier(jnp.max(scores, axis=-1, keepdims=True))
        weights_exp = jnp.exp(scores - top_score)
        exp_total = lax.optimization_barrier(jnp.sum(weights_exp, axis=-1))
        probs = weights_exp.astype(jnp.bfloat16).astype(jnp.float32)
        weighted = jnp.einsum('kgcl,lkv->kgcv', probs, value_rows.astype(jnp.float32))
        attended = weighted / exp_total[..., None]
        difference = attended[:, :, 0] - lam_grid * attended[:, :, 1]
        head_norm = lax.rsqrt(lax.optimization_barrier(jnp.mean(difference * difference, axis=-1, keepdims=True)) + EPS)
        head_out = difference * head_norm * head_gain
        return head_out.reshape(HEADS * VALUE).astype(jnp.bfloat16)
    head_out = lax.map(attend, (rotated, key_cache, value_cache))
    group_rows = HEADS * VALUE // N_TP
    attention = jnp.zeros((BATCH, D), jnp.float32)
    for tp_slot in range(N_TP):
        block_out = lax.dot_general(head_out[:, tp_slot * group_rows:(tp_slot + 1) * group_rows], out_weight[:, tp_slot * group_rows:(tp_slot + 1) * group_rows], (((1,), (1,)), ((), ())), preferred_element_type=jnp.float32).astype(jnp.bfloat16)
        attention = attention + block_out.astype(jnp.float32)
    stream = as_float + attention
    stream_square = lax.optimization_barrier(jnp.mean(stream * stream, axis=-1, keepdims=True))
    normed = (stream * lax.rsqrt(stream_square + EPS) * mlp_gain).astype(jnp.bfloat16)
    gate_out = lax.dot_general(normed, gate_weight, (((1,), (1,)), ((), ())), preferred_element_type=jnp.float32)
    up_out = lax.dot_general(normed, up_weight, (((1,), (1,)), ((), ())), preferred_element_type=jnp.float32)
    hidden = (jax.nn.silu(gate_out) * up_out).astype(jnp.bfloat16)
    down_out = jnp.dot(hidden, down_weight, preferred_element_type=jnp.float32)
    return (stream + down_out).astype(jnp.bfloat16)
```

```python
import functools

import jax
import jax.numpy as jnp
import numpy as np
from jax import lax
from jax.experimental import pallas as pl
from jax.experimental.pallas import tpu as pltpu
from jax.sharding import PartitionSpec as P

EPS = 1e-06
THETA = 10000.0
LANES = 128


def merged(x, axis, combine):
    everything = jax.tree.map(lambda part: lax.all_gather(part, axis), x)
    first = jax.tree.map(lambda part: part[0], everything)

    def hop(k, so_far):
        return combine(so_far, jax.tree.map(lambda part: part[k], everything))

    return lax.fori_loop(1, lax.axis_size(axis), hop, first)


def rotate(vector, position):
    half_len = vector.shape[-1] // 2
    inv_freq = 1.0 / THETA ** (jnp.arange(half_len, dtype=jnp.float32) / half_len)
    angles = position * inv_freq
    cos_table = jnp.cos(angles)
    sin_table = jnp.sin(angles)
    first_half = vector[..., :half_len]
    second_half = vector[..., half_len:]
    return jnp.concatenate(
        [
            first_half * cos_table - second_half * sin_table,
            second_half * cos_table + first_half * sin_table,
        ],
        axis=-1,
    )


def combine(earlier, latter):
    peak_a, total_a, value_a = earlier
    peak_b, total_b, value_b = latter
    peak_new = jnp.maximum(peak_a, peak_b)
    factor_a = jnp.exp(peak_a - peak_new)
    factor_b = jnp.exp(peak_b - peak_new)
    return (
        peak_new,
        total_a * factor_a + total_b * factor_b,
        value_a * factor_a[..., None] + value_b * factor_b[..., None],
    )


def inner_last(left, right):
    return lax.dot_general(
        left, right, (((1,), (1,)), ((), ())), preferred_element_type=jnp.float32
    )


def shards(
    tokens,
    attn_gain,
    query_weight,
    key_cache,
    value_cache,
    head_lambda,
    head_gain,
    out_weight,
    mlp_gain,
    gate_weight,
    up_weight,
    down_weight,
):
    row_count = tokens.shape[0]
    kv_count = lax.axis_size("kv")
    tp_count = lax.axis_size("tp")
    kv_index = lax.axis_index("kv")
    row_span = query_weight.shape[0]
    full_rows = lax.all_gather(tokens, ("kv", "tp"), axis=1, tiled=True)
    wide_rows = full_rows.astype(jnp.float32)
    mean_square = jnp.mean(wide_rows * wide_rows, axis=-1, keepdims=True)
    scaled = (wide_rows * attn_gain).astype(jnp.bfloat16)
    local_cols = lax.dynamic_slice_in_dim(scaled, kv_index * row_span, row_span, 1)
    queries = lax.psum(jnp.dot(local_cols, query_weight, preferred_element_type=jnp.float32), "kv")
    queries = queries * lax.rsqrt(mean_square + EPS)
    head_count = head_lambda.shape[0]
    kv_local = key_cache.shape[2]
    group_size = head_count // kv_local
    position_count = key_cache.shape[1]
    half_dim = key_cache.shape[3] // 2
    value_dim = value_cache.shape[3]
    queries = queries.reshape(row_count, kv_local, group_size, 2, half_dim)
    rotated = rotate(queries, jnp.float32(position_count * kv_count)).astype(jnp.bfloat16)
    key_grid = key_cache.reshape(row_count, position_count, kv_local, 2, half_dim)
    scores = jnp.einsum(
        "bkgch,bpkch->bkgcp", rotated, key_grid, preferred_element_type=jnp.float32
    ) * half_dim ** (-0.5)
    local_peak = jnp.max(scores, axis=-1)
    weights_exp = jnp.exp(scores - local_peak[..., None])
    lam_grid = head_lambda.reshape(kv_local, group_size)[None, :, :, None]
    exp_total = jnp.sum(weights_exp, axis=-1)
    weighted = jnp.einsum(
        "bkgcp,bpkv->bkgcv",
        weights_exp.astype(jnp.bfloat16),
        value_cache,
        preferred_element_type=jnp.float32,
    )
    peak_all, total_all, weighted_all = merged((local_peak, exp_total, weighted), "kv", combine)
    attended = weighted_all / total_all[..., None]
    difference = attended[:, :, :, 0] - lam_grid * attended[:, :, :, 1]
    head_norm = lax.rsqrt(jnp.mean(difference * difference, axis=-1, keepdims=True) + EPS)
    head_out = (difference * head_norm * head_gain).reshape(row_count, head_count * value_dim)
    head_out = head_out.astype(jnp.bfloat16)
    out_part = inner_last(head_out, out_weight).astype(jnp.bfloat16)
    pieces = lax.all_gather(out_part, ("kv", "tp"), axis=1, tiled=True)
    attention = jnp.sum(
        pieces.astype(jnp.float32).reshape(row_count, kv_count, tp_count, -1), axis=2
    )
    stream = wide_rows + attention.reshape(row_count, -1)
    stream_square = jnp.mean(stream * stream, axis=-1, keepdims=True)
    normed = (stream * lax.rsqrt(stream_square + EPS) * mlp_gain).astype(jnp.bfloat16)
    gate_out = inner_last(normed, gate_weight)
    up_out = inner_last(normed, up_weight)
    hidden = (jax.nn.silu(gate_out) * up_out).astype(jnp.bfloat16)
    own_cols = tokens.shape[1]
    down_cols = lax.psum_scatter(
        lax.dot_general(
            down_weight, hidden, (((0,), (1,)), ((), ())), preferred_element_type=jnp.float32
        ),
        ("kv", "tp"),
        scatter_dimension=0,
        tiled=True,
    )
    column_index = lax.axis_index(("kv", "tp"))
    own_stream = lax.dynamic_slice_in_dim(stream, column_index * own_cols, own_cols, 1)
    return (own_stream + down_cols.T).astype(jnp.bfloat16)


def same_chip_kernel(
    kv_n, tp_n, tok, again, wq_h, kc_h, vc_h, lam, hgain, wo_h, mgain, wg_h, wu_h, wd_h, table,
    out,
    wq, kc, vc, wo, wg, wu, wd,
    tg, qs, qr, qf, ms, mr, hs, ho, hf, og, og_r, stream, hid, ds, dr,
    wsem, tsend, trecv, qsend, qrecv, msend, mrecv, hsend, hrecv, osend, orecv, dsend, drecv,
):
    kv, tp = lax.axis_index("kv"), lax.axis_index("tp")
    n_all = kv_n * tp_n
    me = kv * tp_n + tp
    rows, own = tok.shape
    loads = []
    for slot, (src, dst) in enumerate(
        [(wq_h, wq), (kc_h, kc), (vc_h, vc), (wo_h, wo), (wg_h, wg), (wu_h, wu), (wd_h, wd)]
    ):
        load = pltpu.make_async_copy(src, dst, wsem.at[slot])
        load.start()
        loads.append(load)

    def spot(delta):
        other = lax.rem(me + delta, n_all)
        return {"kv": other // tp_n, "tp": lax.rem(other, tp_n)}

    def along(delta):
        return {"kv": lax.rem(kv + delta, kv_n), "tp": tp}

    def remote(src, dst, send, recv, where):
        copy = pltpu.make_async_remote_copy(
            src_ref=src, dst_ref=dst, send_sem=send, recv_sem=recv,
            device_id=where, device_id_type=pl.DeviceIdType.MESH,
        )
        copy.start()
        return copy

    barrier = pltpu.get_barrier_semaphore()
    for delta in range(1, n_all):
        pl.semaphore_signal(
            barrier, inc=1, device_id=spot(delta), device_id_type=pl.DeviceIdType.MESH
        )
    tg[me] = tok[...]
    pl.semaphore_wait(barrier, n_all - 1)
    sends = []

    mate = {"kv": kv, "tp": lax.rem(tp + 1, tp_n)}
    pair = remote(tok, tg.at[me], tsend.at[0], trecv.at[0], mate)
    token_copies = [pair]
    for delta in range(1, kv_n):
        for across in range(tp_n):
            where = {"kv": lax.rem(kv + delta, kv_n), "tp": lax.rem(tp + across, tp_n)}
            slot = delta * tp_n + across
            token_copies.append(remote(tok, tg.at[me], tsend.at[slot], trecv.at[slot], where))
    sends += token_copies

    pair.wait_recv()
    parts = []
    for half in range(tp_n):
        at = kv * tp_n + half
        gain = again[:, pl.ds(pl.multiple_of(at * own, LANES), own)]
        parts.append((tg[at].astype(jnp.float32) * gain).astype(jnp.bfloat16))
    scaled = jnp.concatenate(parts, axis=1)
    loads[0].wait()
    head_count = qs.shape[0]
    value_dim = qs.shape[2]
    per = 4
    pieces = head_count // per
    query_copies = []
    for j in range(pieces):
        width = per * value_dim
        product = jnp.dot(
            scaled, wq[:, j * width:(j + 1) * width], preferred_element_type=jnp.float32
        )
        for i in range(per):
            qs[j * per + i] = product[:, i * value_dim:(i + 1) * value_dim]
        for delta in range(1, kv_n):
            part = pl.ds(j * per, per)
            query_copies.append(
                remote(
                    qs.at[part], qr.at[delta - 1, part],
                    qsend.at[j, delta - 1], qrecv.at[j, delta - 1], along(delta),
                )
            )
    sends += query_copies

    for copy in token_copies[1:]:
        copy.wait_recv()
    square = jnp.zeros((rows, 1), jnp.float32)
    for at in range(n_all):
        wide = tg[at].astype(jnp.float32)
        square = square + jnp.sum(wide * wide, axis=1, keepdims=True)
    scale = lax.rsqrt(square / (n_all * own) + EPS)

    for copy in query_copies:
        copy.wait_recv()
    lane = lax.broadcasted_iota(jnp.int32, (rows, value_dim), 1)
    half = value_dim // 2
    first = lax.rem(lane, half) < half // 2
    cosines = table[0:1, :]
    sines = table[1:2, :]
    for h in range(head_count):
        total = qs[h]
        for delta in range(1, kv_n):
            total = total + qr[delta - 1, h]
        total = total * scale
        swapped = jnp.where(
            first,
            pltpu.roll(total, value_dim - half // 2, 1),
            pltpu.roll(total, half // 2, 1),
        )
        qf[h] = total * cosines + swapped * sines

    loads[1].wait()
    loads[2].wait()
    both = 2 * head_count
    low = lax.broadcasted_iota(jnp.int32, (head_count, value_dim), 1) < half
    row_at = lax.broadcasted_iota(jnp.int32, (both, value_dim), 0)
    lane_at = lax.broadcasted_iota(jnp.int32, (both, value_dim), 1)
    for b in range(rows):
        query = qf[:, b, :]
        grid = jnp.concatenate(
            [jnp.where(low, query, 0.0), jnp.where(low, 0.0, query)], axis=0
        ).astype(jnp.bfloat16)
        scores = inner_last(grid, kc[b]) * half ** (-0.5)
        peak = jnp.max(scores, axis=1, keepdims=True)
        exps = jnp.exp(scores - peak)
        sums = jnp.sum(exps, axis=1, keepdims=True)
        ms[b, 0:both, :] = jnp.dot(
            exps.astype(jnp.bfloat16), vc[b], preferred_element_type=jnp.float32
        )
        stats = jnp.where(lane_at == row_at, peak, 0.0) + jnp.where(
            lane_at == row_at + both, sums, 0.0
        )
        ms[b, both:both + 8, :] = jnp.broadcast_to(
            jnp.sum(stats, axis=0, keepdims=True), (8, value_dim)
        )

    merge_copies = []
    for delta in range(1, kv_n):
        other = lax.rem(kv + delta, kv_n)
        merge_copies.append(
            remote(
                ms.at[other], mr.at[delta - 1],
                msend.at[delta - 1], mrecv.at[delta - 1], along(delta),
            )
        )
    sends += merge_copies

    lam_at = lax.broadcasted_iota(jnp.int32, (head_count, head_count), 0)
    lam_lane = lax.broadcasted_iota(jnp.int32, (head_count, head_count), 1)
    lam_col = jnp.sum(
        jnp.where(lam_at == lam_lane, lam[...], 0.0), axis=1, keepdims=True
    )
    for copy in merge_copies:
        copy.wait_recv()
    gathered = []
    for source in range(kv_n):
        block = ms[kv] if source == 0 else mr[source - 1]
        stats = block[both:both + 1, :]
        peak = jnp.sum(jnp.where(lane_at == row_at, stats, 0.0), axis=1, keepdims=True)
        sums = jnp.sum(jnp.where(lane_at == row_at + both, stats, 0.0), axis=1, keepdims=True)
        gathered.append((peak, sums, block[0:both, :]))
    top = gathered[0][0]
    for peak, _, _ in gathered[1:]:
        top = jnp.maximum(top, peak)
    all_sums = jnp.zeros_like(top)
    weighted = jnp.zeros((both, value_dim), jnp.float32)
    for peak, sums, values in gathered:
        factor = jnp.exp(peak - top)
        all_sums = all_sums + sums * factor
        weighted = weighted + values * factor
    attended = weighted / all_sums
    difference = attended[0:head_count] - lam_col * attended[head_count:both]
    norm = lax.rsqrt(jnp.mean(difference * difference, axis=1, keepdims=True) + EPS)
    head_out = (difference * norm * hgain[...]).astype(jnp.bfloat16)
    hs[...] = head_out
    ho[kv] = head_out
    head_copies = []
    for delta in range(1, kv_n):
        head_copies.append(
            remote(hs, ho.at[kv], hsend.at[delta - 1], hrecv.at[delta - 1], along(delta))
        )
    sends += head_copies
    for copy in head_copies:
        copy.wait_recv()
    for b in range(rows):
        hf[b] = ho[b].astype(jnp.float32)
    flat = jnp.concatenate(
        [hf[:, h, :] for h in range(head_count)], axis=1
    ).astype(jnp.bfloat16)
    loads[3].wait()
    features = wo.shape[0]
    width = 256
    for j in range(features // width):
        part = inner_last(flat, wo[j * width:(j + 1) * width, :]).astype(jnp.bfloat16)
        og[:, j * width:(j + 1) * width] = part
    og_r[me] = og[...]
    out_copies = []
    for delta in range(1, n_all):
        out_copies.append(
            remote(og, og_r.at[me], osend.at[delta - 1], orecv.at[delta - 1], spot(delta))
        )
    sends += out_copies
    for copy in out_copies:
        copy.wait_recv()
    square = jnp.zeros((rows, 1), jnp.float32)
    for at in range(kv_n):
        tokens = jnp.concatenate(
            [tg[at * tp_n + g].astype(jnp.float32) for g in range(tp_n)], axis=1
        )
        attention = og_r[at * tp_n].astype(jnp.float32)
        for g in range(1, tp_n):
            attention = attention + og_r[at * tp_n + g].astype(jnp.float32)
        piece = tokens + attention
        stream[:, at * features:(at + 1) * features] = piece
        square = square + jnp.sum(piece * piece, axis=1, keepdims=True)
    scale = lax.rsqrt(square / (n_all * own) + EPS)
    normed = (stream[...] * scale * mgain[...]).astype(jnp.bfloat16)

    loads[4].wait()
    loads[5].wait()
    units = wg.shape[0]
    step = LANES

    def unit_block(j, carry):
        at = pl.ds(pl.multiple_of(j * step, step), step)
        gate = inner_last(normed, wg[at, :])
        up = inner_last(normed, wu[at, :])
        hid[:, at] = (gate / (1.0 + jnp.exp(-gate)) * up).astype(jnp.bfloat16)
        return carry

    lax.fori_loop(0, units // step, unit_block, 0)
    hidden = hid[...]
    loads[6].wait()
    order = [n_all // 2 + (i + 1) // 2 * (1 if i % 2 else -1) for i in range(n_all)]
    order = [d for d in order if 0 < d < n_all] + [0]
    down_copies = []
    mine = None
    for delta in order:
        at = lax.rem(me + delta, n_all)
        block = jnp.dot(
            hidden,
            wd[:, pl.ds(pl.multiple_of(at * own, LANES), own)],
            preferred_element_type=jnp.float32,
        )
        if delta == 0:
            mine = block
        else:
            ds[delta - 1] = block
            down_copies.append(
                remote(
                    ds.at[delta - 1], dr.at[delta - 1],
                    dsend.at[delta - 1], drecv.at[delta - 1], spot(delta),
                )
            )
    sends += down_copies
    total = mine
    for copy in down_copies:
        copy.wait_recv()
    for delta in range(1, n_all):
        total = total + dr[delta - 1]
    mixed = stream[:, pl.ds(pl.multiple_of(me * own, LANES), own)] + total
    out[...] = mixed.astype(out.dtype)
    for copy in sends:
        copy.wait_send()


def turning(head_dim, position):
    half_len = head_dim // 4
    inv_freq = np.float32(1.0) / np.float32(THETA) ** (
        np.arange(half_len, dtype=np.float32) / np.float32(half_len)
    )
    angles = (np.float32(position) * inv_freq.astype(np.float32)).astype(np.float32)
    cos, sin = np.cos(angles), np.sin(angles)
    return np.stack(
        [np.concatenate([cos, cos] * 2), np.concatenate([-sin, sin] * 2)]
    ).astype(np.float32)


def fused(kv_n, tp_n, *arrays):
    (tokens, attn_gain, wq, kc, vc, lam, hgain, wo, mgain, wg, wu, wd) = arrays
    rows, own = tokens.shape
    n_all = kv_n * tp_n
    positions, value_dim = kc.shape[1], kc.shape[3]
    heads = lam.shape[0]
    both = 2 * heads
    model = n_all * own
    f32, bf16 = jnp.float32, jnp.bfloat16
    table = jnp.asarray(turning(value_dim, positions * kv_n))
    dma = pltpu.SemaphoreType.DMA
    vmem = pl.BlockSpec(memory_space=pltpu.VMEM)
    hbm = pl.BlockSpec(memory_space=pl.ANY)
    return pl.pallas_call(
        functools.partial(same_chip_kernel, kv_n, tp_n),
        out_shape=jax.ShapeDtypeStruct((rows, own), tokens.dtype),
        in_specs=[vmem, vmem, hbm, hbm, hbm, vmem, vmem, hbm, vmem, hbm, hbm, hbm, vmem],
        out_specs=vmem,
        scratch_shapes=[
            pltpu.VMEM(wq.shape, bf16),
            pltpu.VMEM((rows, positions, value_dim), bf16),
            pltpu.VMEM((rows, positions, value_dim), bf16),
            pltpu.VMEM(wo.shape, bf16),
            pltpu.VMEM(wg.shape, bf16),
            pltpu.VMEM(wu.shape, bf16),
            pltpu.VMEM(wd.shape, bf16),
            pltpu.VMEM((n_all, rows, own), bf16),
            pltpu.VMEM((heads, rows, value_dim), f32),
            pltpu.VMEM((kv_n - 1, heads, rows, value_dim), f32),
            pltpu.VMEM((heads, rows, value_dim), f32),
            pltpu.VMEM((rows, both + 8, value_dim), f32),
            pltpu.VMEM((kv_n - 1, both + 8, value_dim), f32),
            pltpu.VMEM((heads, value_dim), bf16),
            pltpu.VMEM((rows, heads, value_dim), bf16),
            pltpu.VMEM((rows, heads, value_dim), f32),
            pltpu.VMEM((rows, wo.shape[0]), bf16),
            pltpu.VMEM((n_all, rows, wo.shape[0]), bf16),
            pltpu.VMEM((rows, model), f32),
            pltpu.VMEM((rows, wg.shape[0]), bf16),
            pltpu.VMEM((n_all - 1, rows, own), f32),
            pltpu.VMEM((n_all - 1, rows, own), f32),
            dma((7,)),
            dma((n_all,)), dma((n_all,)),
            dma((heads // 4, kv_n - 1)), dma((heads // 4, kv_n - 1)),
            dma((kv_n - 1,)), dma((kv_n - 1,)),
            dma((kv_n - 1,)), dma((kv_n - 1,)),
            dma((n_all - 1,)), dma((n_all - 1,)),
            dma((n_all - 1,)), dma((n_all - 1,)),
        ],
        compiler_params=pltpu.CompilerParams(
            collective_id=0, has_side_effects=True, vmem_limit_bytes=67043328
        ),
    )(
        tokens, attn_gain.reshape(1, -1), wq,
        kc.reshape(rows, positions, value_dim), vc.reshape(rows, positions, value_dim),
        lam.reshape(1, -1), hgain.reshape(1, -1), wo, mgain.reshape(1, -1), wg, wu, wd, table,
    )


def layer(kv_n, tp_n, *arrays):
    tokens, kc, wg = arrays[0], arrays[3], arrays[9]
    small = tokens.shape[0] == kv_n and kc.shape[2] == 1 and tp_n == 2
    if small and tokens.shape[1] % LANES == 0 and wg.shape[0] % LANES == 0:
        return fused(kv_n, tp_n, *arrays)
    return shards(*arrays)


def solution(mesh):
    placed = (
        P("dp", ("kv", "tp")),
        P(),
        P("kv", "tp"),
        P("dp", "kv", "tp", None),
        P("dp", "kv", "tp", None),
        P("tp"),
        P(),
        P("kv", "tp"),
        P(),
        P(("kv", "tp"), None),
        P(("kv", "tp"), None),
        P(("kv", "tp"), None),
    )
    return jax.shard_map(
        functools.partial(layer, mesh.shape["kv"], mesh.shape["tp"]),
        mesh=mesh, in_specs=placed, out_specs=P("dp", ("kv", "tp")), check_vma=False
    )
```

```python
import functools

import jax
import jax.numpy as jnp
import numpy as np
from jax import lax
from jax.experimental import pallas as pl
from jax.experimental.pallas import tpu as pltpu
from jax.sharding import PartitionSpec as P

EPS = 1e-06
THETA = 10000.0
LANES = 128
CUTS = (5, 13, 22)


def merged(x, axis, combine):
    everything = jax.tree.map(lambda part: lax.all_gather(part, axis), x)
    first = jax.tree.map(lambda part: part[0], everything)

    def hop(k, so_far):
        return combine(so_far, jax.tree.map(lambda part: part[k], everything))

    return lax.fori_loop(1, lax.axis_size(axis), hop, first)


def rotate(vector, position):
    half_len = vector.shape[-1] // 2
    inv_freq = 1.0 / THETA ** (jnp.arange(half_len, dtype=jnp.float32) / half_len)
    angles = position * inv_freq
    cos_table = jnp.cos(angles)
    sin_table = jnp.sin(angles)
    first_half = vector[..., :half_len]
    second_half = vector[..., half_len:]
    return jnp.concatenate(
        [
            first_half * cos_table - second_half * sin_table,
            second_half * cos_table + first_half * sin_table,
        ],
        axis=-1,
    )


def combine(earlier, latter):
    peak_a, total_a, value_a = earlier
    peak_b, total_b, value_b = latter
    peak_new = jnp.maximum(peak_a, peak_b)
    factor_a = jnp.exp(peak_a - peak_new)
    factor_b = jnp.exp(peak_b - peak_new)
    return (
        peak_new,
        total_a * factor_a + total_b * factor_b,
        value_a * factor_a[..., None] + value_b * factor_b[..., None],
    )


def inner_last(left, right):
    return lax.dot_general(
        left, right, (((1,), (1,)), ((), ())), preferred_element_type=jnp.float32
    )


def shards(
    tokens,
    attn_gain,
    query_weight,
    key_cache,
    value_cache,
    head_lambda,
    head_gain,
    out_weight,
    mlp_gain,
    gate_weight,
    up_weight,
    down_weight,
):
    row_count = tokens.shape[0]
    kv_count = lax.axis_size("kv")
    tp_count = lax.axis_size("tp")
    kv_index = lax.axis_index("kv")
    row_span = query_weight.shape[0]
    full_rows = lax.all_gather(tokens, ("kv", "tp"), axis=1, tiled=True)
    wide_rows = full_rows.astype(jnp.float32)
    mean_square = jnp.mean(wide_rows * wide_rows, axis=-1, keepdims=True)
    scaled = (wide_rows * attn_gain).astype(jnp.bfloat16)
    local_cols = lax.dynamic_slice_in_dim(scaled, kv_index * row_span, row_span, 1)
    queries = lax.psum(jnp.dot(local_cols, query_weight, preferred_element_type=jnp.float32), "kv")
    queries = queries * lax.rsqrt(mean_square + EPS)
    head_count = head_lambda.shape[0]
    kv_local = key_cache.shape[2]
    group_size = head_count // kv_local
    position_count = key_cache.shape[1]
    half_dim = key_cache.shape[3] // 2
    value_dim = value_cache.shape[3]
    queries = queries.reshape(row_count, kv_local, group_size, 2, half_dim)
    rotated = rotate(queries, jnp.float32(position_count * kv_count)).astype(jnp.bfloat16)
    key_grid = key_cache.reshape(row_count, position_count, kv_local, 2, half_dim)
    scores = jnp.einsum(
        "bkgch,bpkch->bkgcp", rotated, key_grid, preferred_element_type=jnp.float32
    ) * half_dim ** (-0.5)
    local_peak = jnp.max(scores, axis=-1)
    weights_exp = jnp.exp(scores - local_peak[..., None])
    lam_grid = head_lambda.reshape(kv_local, group_size)[None, :, :, None]
    exp_total = jnp.sum(weights_exp, axis=-1)
    weighted = jnp.einsum(
        "bkgcp,bpkv->bkgcv",
        weights_exp.astype(jnp.bfloat16),
        value_cache,
        preferred_element_type=jnp.float32,
    )
    peak_all, total_all, weighted_all = merged((local_peak, exp_total, weighted), "kv", combine)
    attended = weighted_all / total_all[..., None]
    difference = attended[:, :, :, 0] - lam_grid * attended[:, :, :, 1]
    head_norm = lax.rsqrt(jnp.mean(difference * difference, axis=-1, keepdims=True) + EPS)
    head_out = (difference * head_norm * head_gain).reshape(row_count, head_count * value_dim)
    head_out = head_out.astype(jnp.bfloat16)
    out_part = inner_last(head_out, out_weight).astype(jnp.bfloat16)
    pieces = lax.all_gather(out_part, ("kv", "tp"), axis=1, tiled=True)
    attention = jnp.sum(
        pieces.astype(jnp.float32).reshape(row_count, kv_count, tp_count, -1), axis=2
    )
    stream = wide_rows + attention.reshape(row_count, -1)
    stream_square = jnp.mean(stream * stream, axis=-1, keepdims=True)
    normed = (stream * lax.rsqrt(stream_square + EPS) * mlp_gain).astype(jnp.bfloat16)
    gate_out = inner_last(normed, gate_weight)
    up_out = inner_last(normed, up_weight)
    hidden = (jax.nn.silu(gate_out) * up_out).astype(jnp.bfloat16)
    own_cols = tokens.shape[1]
    down_cols = lax.psum_scatter(
        lax.dot_general(
            down_weight, hidden, (((0,), (1,)), ((), ())), preferred_element_type=jnp.float32
        ),
        ("kv", "tp"),
        scatter_dimension=0,
        tiled=True,
    )
    column_index = lax.axis_index(("kv", "tp"))
    own_stream = lax.dynamic_slice_in_dim(stream, column_index * own_cols, own_cols, 1)
    return (own_stream + down_cols.T).astype(jnp.bfloat16)


def same_chip_kernel(
    kv_n, tp_n, tok, again, wq_h, kc_h, vc_h, lam, hgain, wo_h, mgain, wg_h, wu_h, wd_h, table,
    out,
    wq, kc, vc, wo, stage, wgu_t, wd,
    tg, qs, qr, qf, ms, mb, mr, st, sr, hf, og, og_r, stream, hid, ds, dr,
    wsem, csem, tsend, trecv, qsend, qrecv, msend, mrecv, hsend, hrecv, osend, orecv, dsend, drecv,
):
    kv, tp = lax.axis_index("kv"), lax.axis_index("tp")
    n_all = kv_n * tp_n
    me = kv * tp_n + tp
    rows, own = tok.shape
    loads = []
    for slot, (src, dst) in enumerate(
        [(wq_h, wq), (kc_h, kc), (vc_h, vc), (wo_h, wo)]
    ):
        load = pltpu.make_async_copy(src, dst, wsem.at[slot])
        load.start()
        loads.append(load)
    features = wo.shape[0]
    units = wg_h.shape[0]
    per_weight = units // LANES
    chunks = 2 * per_weight
    slots = stage.shape[0]

    def chunk_load(weight, i, slot):
        piece = pl.ds(pl.multiple_of(i * LANES, LANES), LANES)
        at = i if weight is wg_h else i + per_weight
        return pltpu.make_async_copy(weight.at[piece], stage.at[slot], csem.at[at])

    for g in range(slots):
        if g < per_weight:
            chunk_load(wg_h, g, g).start()
        else:
            chunk_load(wu_h, g - per_weight, g).start()

    def turn(low, high):
        def turn_gate(i, carry):
            slot = lax.rem(i, slots)
            chunk_load(wg_h, i, slot).wait()
            at = pl.ds(pl.multiple_of(i * LANES, LANES), LANES)
            wgu_t[0, :, at] = stage[slot].T

            @pl.when(i + slots < chunks)
            def _():
                chunk_load(wu_h, i + slots - per_weight, slot).start()

            return carry

        def turn_up(i, carry):
            slot = lax.rem(i + per_weight, slots)
            chunk_load(wu_h, i, slot).wait()
            at = pl.ds(pl.multiple_of(i * LANES, LANES), LANES)
            wgu_t[1, :, at] = stage[slot].T
            return carry

        low, high = chunks * low // 22, chunks * high // 22
        if low < per_weight:
            lax.fori_loop(low, min(high, per_weight), turn_gate, 0)
        if high > per_weight:
            lax.fori_loop(max(low, per_weight) - per_weight, high - per_weight, turn_up, 0)

    down_load = pltpu.make_async_copy(wd_h, wd, wsem.at[4])
    down_load.start()

    def spot(delta):
        other = lax.rem(me + delta, n_all)
        return {"kv": other // tp_n, "tp": lax.rem(other, tp_n)}

    def along(delta):
        return {"kv": lax.rem(kv + delta, kv_n), "tp": tp}

    def remote(src, dst, send, recv, where):
        copy = pltpu.make_async_remote_copy(
            src_ref=src, dst_ref=dst, send_sem=send, recv_sem=recv,
            device_id=where, device_id_type=pl.DeviceIdType.MESH,
        )
        copy.start()
        return copy

    barrier = pltpu.get_barrier_semaphore()
    for delta in range(1, n_all):
        pl.semaphore_signal(
            barrier, inc=1, device_id=spot(delta), device_id_type=pl.DeviceIdType.MESH
        )
    tg[me] = tok[...]
    pl.semaphore_wait(barrier, n_all - 1)
    sends = []

    mate = {"kv": kv, "tp": lax.rem(tp + 1, tp_n)}
    pair = remote(tok, tg.at[me], tsend.at[0], trecv.at[0], mate)
    token_copies = [pair]
    for delta in range(1, kv_n):
        for across in range(tp_n):
            where = {"kv": lax.rem(kv + delta, kv_n), "tp": lax.rem(tp + across, tp_n)}
            slot = delta * tp_n + across
            token_copies.append(remote(tok, tg.at[me], tsend.at[slot], trecv.at[slot], where))
    sends += token_copies

    pair.wait_recv()
    parts = []
    for half in range(tp_n):
        at = kv * tp_n + half
        gain = again[:, pl.ds(pl.multiple_of(at * own, LANES), own)]
        parts.append((tg[at].astype(jnp.float32) * gain).astype(jnp.bfloat16))
    scaled = jnp.concatenate(parts, axis=1)
    loads[0].wait()
    head_count = qs.shape[0]
    value_dim = qs.shape[2]
    per = 4
    pieces = head_count // per
    query_copies = []
    for j in range(pieces):
        width = per * value_dim
        product = jnp.dot(
            scaled, wq[:, j * width:(j + 1) * width], preferred_element_type=jnp.float32
        )
        for i in range(per):
            qs[j * per + i] = product[:, i * value_dim:(i + 1) * value_dim]
        for delta in range(1, kv_n):
            part = pl.ds(j * per, per)
            query_copies.append(
                remote(
                    qs.at[part], qr.at[delta - 1, part],
                    qsend.at[j, delta - 1], qrecv.at[j, delta - 1], along(delta),
                )
            )
    sends += query_copies

    for copy in token_copies[1:]:
        copy.wait_recv()
    square = jnp.zeros((rows, 1), jnp.float32)
    for at in range(n_all):
        wide = tg[at].astype(jnp.float32)
        square = square + jnp.sum(wide * wide, axis=1, keepdims=True)
    scale = lax.rsqrt(square / (n_all * own) + EPS)

    turn(0, CUTS[0])
    for copy in query_copies:
        copy.wait_recv()
    lane = lax.broadcasted_iota(jnp.int32, (rows, value_dim), 1)
    half = value_dim // 2
    first = lax.rem(lane, half) < half // 2
    cosines = table[0:1, :]
    sines = table[1:2, :]
    for h in range(head_count):
        total = qs[h]
        for delta in range(1, kv_n):
            total = total + qr[delta - 1, h]
        total = total * scale
        swapped = jnp.where(
            first,
            pltpu.roll(total, value_dim - half // 2, 1),
            pltpu.roll(total, half // 2, 1),
        )
        qf[h] = total * cosines + swapped * sines

    loads[1].wait()
    loads[2].wait()
    both = 2 * head_count
    low = lax.broadcasted_iota(jnp.int32, (head_count, value_dim), 1) < half
    row_at = lax.broadcasted_iota(jnp.int32, (both, value_dim), 0)
    lane_at = lax.broadcasted_iota(jnp.int32, (both, value_dim), 1)
    spread = []
    for b in range(rows):
        query = qf[:, b, :]
        grid = jnp.concatenate(
            [jnp.where(low, query, 0.0), jnp.where(low, 0.0, query)], axis=0
        ).astype(jnp.bfloat16)
        scores = inner_last(grid, kc[b]) * half ** (-0.5)
        peak = jnp.max(scores, axis=1, keepdims=True)
        exps = jnp.exp(scores - peak)
        sums = jnp.sum(exps, axis=1, keepdims=True)
        spread.append(exps.astype(jnp.bfloat16))
        stats = jnp.where(lane_at == row_at, peak, 0.0) + jnp.where(
            lane_at == row_at + both, sums, 0.0
        )
        st[b:b + 1, :] = jnp.sum(stats, axis=0, keepdims=True)
    stat_copies = []
    for delta in range(1, kv_n):
        stat_copies.append(
            remote(
                st, sr.at[delta - 1], hsend.at[delta - 1], hrecv.at[delta - 1], along(delta)
            )
        )
    merge_copies = []
    for b in range(rows):
        values = jnp.dot(spread[b], vc[b], preferred_element_type=jnp.float32)
        ms[b] = values
        mb[b] = values.astype(jnp.bfloat16)
        for delta in range(1, kv_n):
            merge_copies.append(
                remote(
                    mb.at[b], mr.at[delta - 1, b],
                    msend.at[b, delta - 1], mrecv.at[b, delta - 1], along(delta),
                )
            )
    sends += stat_copies + merge_copies

    lam_at = lax.broadcasted_iota(jnp.int32, (head_count, head_count), 0)
    lam_lane = lax.broadcasted_iota(jnp.int32, (head_count, head_count), 1)
    lam_col = jnp.sum(
        jnp.where(lam_at == lam_lane, lam[...], 0.0), axis=1, keepdims=True
    )
    turn(CUTS[0], CUTS[1])
    for copy in stat_copies:
        copy.wait_recv()
    for b in range(rows):
        for copy in merge_copies[b * (kv_n - 1):(b + 1) * (kv_n - 1)]:
            copy.wait_recv()
        gathered = []
        for source in range(kv_n):
            stats = st[b:b + 1, :] if source == 0 else sr[source - 1, b:b + 1, :]
            values = ms[b] if source == 0 else mr[source - 1, b].astype(jnp.float32)
            peak = jnp.sum(jnp.where(lane_at == row_at, stats, 0.0), axis=1, keepdims=True)
            sums = jnp.sum(
                jnp.where(lane_at == row_at + both, stats, 0.0), axis=1, keepdims=True
            )
            gathered.append((peak, sums, values))
        top = gathered[0][0]
        for peak, _, _ in gathered[1:]:
            top = jnp.maximum(top, peak)
        all_sums = jnp.zeros_like(top)
        weighted = jnp.zeros((both, value_dim), jnp.float32)
        for peak, sums, values in gathered:
            factor = jnp.exp(peak - top)
            all_sums = all_sums + sums * factor
            weighted = weighted + values * factor
        attended = weighted / all_sums
        difference = attended[0:head_count] - lam_col * attended[head_count:both]
        norm = lax.rsqrt(jnp.mean(difference * difference, axis=1, keepdims=True) + EPS)
        hf[b] = difference * norm * hgain[...]
    flat = jnp.concatenate(
        [hf[:, h, :] for h in range(head_count)], axis=1
    ).astype(jnp.bfloat16)
    loads[3].wait()
    width = 256
    for j in range(features // width):
        part = inner_last(flat, wo[j * width:(j + 1) * width, :]).astype(jnp.bfloat16)
        og[:, j * width:(j + 1) * width] = part
    og_r[me] = og[...]
    out_copies = []
    for delta in range(1, n_all):
        out_copies.append(
            remote(og, og_r.at[me], osend.at[delta - 1], orecv.at[delta - 1], spot(delta))
        )
    sends += out_copies
    turn(CUTS[1], CUTS[2])
    for copy in out_copies:
        copy.wait_recv()
    square = jnp.zeros((rows, 1), jnp.float32)
    for at in range(kv_n):
        tokens = jnp.concatenate(
            [tg[at * tp_n + g].astype(jnp.float32) for g in range(tp_n)], axis=1
        )
        attention = og_r[at * tp_n].astype(jnp.float32)
        for g in range(1, tp_n):
            attention = attention + og_r[at * tp_n + g].astype(jnp.float32)
        piece = tokens + attention
        stream[:, at * features:(at + 1) * features] = piece
        square = square + jnp.sum(piece * piece, axis=1, keepdims=True)
    scale = lax.rsqrt(square / (n_all * own) + EPS)
    normed = (stream[...] * scale * mgain[...]).astype(jnp.bfloat16)

    step = 2 * LANES
    for low in range(0, units, step):
        at = slice(low, min(low + step, units))
        gate = jnp.dot(normed, wgu_t[0, :, at], preferred_element_type=jnp.float32)
        up = jnp.dot(normed, wgu_t[1, :, at], preferred_element_type=jnp.float32)
        hid[:, at] = (gate / (1.0 + jnp.exp(-gate)) * up).astype(jnp.bfloat16)
    hidden = hid[...]
    down_load.wait()
    order = [n_all // 2 + (i + 1) // 2 * (1 if i % 2 else -1) for i in range(n_all)]
    order = [d for d in order if 0 < d < n_all] + [0]
    down_copies = []
    mine = None
    for delta in order:
        at = lax.rem(me + delta, n_all)
        block = jnp.dot(
            hidden,
            wd[:, pl.ds(pl.multiple_of(at * own, LANES), own)],
            preferred_element_type=jnp.float32,
        )
        if delta == 0:
            mine = block
        else:
            ds[delta - 1] = block.astype(ds.dtype)
            down_copies.append(
                remote(
                    ds.at[delta - 1], dr.at[delta - 1],
                    dsend.at[delta - 1], drecv.at[delta - 1], spot(delta),
                )
            )
    sends += down_copies
    total = mine
    for copy in down_copies:
        copy.wait_recv()
    for delta in range(1, n_all):
        total = total + dr[delta - 1].astype(jnp.float32)
    mixed = stream[:, pl.ds(pl.multiple_of(me * own, LANES), own)] + total
    out[...] = mixed.astype(out.dtype)
    for copy in sends:
        copy.wait_send()


def turning(head_dim, position):
    half_len = head_dim // 4
    inv_freq = np.float32(1.0) / np.float32(THETA) ** (
        np.arange(half_len, dtype=np.float32) / np.float32(half_len)
    )
    angles = (np.float32(position) * inv_freq.astype(np.float32)).astype(np.float32)
    cos, sin = np.cos(angles), np.sin(angles)
    return np.stack(
        [np.concatenate([cos, cos] * 2), np.concatenate([-sin, sin] * 2)]
    ).astype(np.float32)


def fused(kv_n, tp_n, *arrays):
    (tokens, attn_gain, wq, kc, vc, lam, hgain, wo, mgain, wg, wu, wd) = arrays
    rows, own = tokens.shape
    n_all = kv_n * tp_n
    positions, value_dim = kc.shape[1], kc.shape[3]
    heads = lam.shape[0]
    both = 2 * heads
    model = n_all * own
    per_weight = wg.shape[0] // LANES
    f32, bf16 = jnp.float32, jnp.bfloat16
    table = jnp.asarray(turning(value_dim, positions * kv_n))
    dma = pltpu.SemaphoreType.DMA
    vmem = pl.BlockSpec(memory_space=pltpu.VMEM)
    hbm = pl.BlockSpec(memory_space=pl.ANY)
    return pl.pallas_call(
        functools.partial(same_chip_kernel, kv_n, tp_n),
        out_shape=jax.ShapeDtypeStruct((rows, own), tokens.dtype),
        in_specs=[vmem, vmem, hbm, hbm, hbm, vmem, vmem, hbm, vmem, hbm, hbm, hbm, vmem],
        out_specs=vmem,
        scratch_shapes=[
            pltpu.VMEM(wq.shape, bf16),
            pltpu.VMEM((rows, positions, value_dim), bf16),
            pltpu.VMEM((rows, positions, value_dim), bf16),
            pltpu.VMEM(wo.shape, bf16),
            pltpu.VMEM((min(per_weight + 5, 2 * per_weight), LANES, model), bf16),
            pltpu.VMEM((2,) + wg.shape[::-1], bf16),
            pltpu.VMEM(wd.shape, bf16),
            pltpu.VMEM((n_all, rows, own), bf16),
            pltpu.VMEM((heads, rows, value_dim), f32),
            pltpu.VMEM((kv_n - 1, heads, rows, value_dim), f32),
            pltpu.VMEM((heads, rows, value_dim), f32),
            pltpu.VMEM((rows, both, value_dim), f32),
            pltpu.VMEM((rows, both, value_dim), bf16),
            pltpu.VMEM((kv_n - 1, rows, both, value_dim), bf16),
            pltpu.VMEM((rows, value_dim), f32),
            pltpu.VMEM((kv_n - 1, rows, value_dim), f32),
            pltpu.VMEM((rows, heads, value_dim), f32),
            pltpu.VMEM((rows, wo.shape[0]), bf16),
            pltpu.VMEM((n_all, rows, wo.shape[0]), bf16),
            pltpu.VMEM((rows, model), f32),
            pltpu.VMEM((rows, wg.shape[0]), bf16),
            pltpu.VMEM((n_all - 1, rows, own), bf16),
            pltpu.VMEM((n_all - 1, rows, own), bf16),
            dma((5,)), dma((2 * per_weight,)),
            dma((n_all,)), dma((n_all,)),
            dma((heads // 4, kv_n - 1)), dma((heads // 4, kv_n - 1)),
            dma((rows, kv_n - 1)), dma((rows, kv_n - 1)),
            dma((kv_n - 1,)), dma((kv_n - 1,)),
            dma((n_all - 1,)), dma((n_all - 1,)),
            dma((n_all - 1,)), dma((n_all - 1,)),
        ],
        compiler_params=pltpu.CompilerParams(
            collective_id=0, has_side_effects=True, vmem_limit_bytes=67043328
        ),
    )(
        tokens, attn_gain.reshape(1, -1), wq,
        kc.reshape(rows, positions, value_dim), vc.reshape(rows, positions, value_dim),
        lam.reshape(1, -1), hgain.reshape(1, -1), wo, mgain.reshape(1, -1), wg, wu, wd, table,
    )


def layer(kv_n, tp_n, *arrays):
    tokens, kc, wg = arrays[0], arrays[3], arrays[9]
    small = tokens.shape[0] == kv_n and kc.shape[2] == 1 and tp_n == 2
    if small and tokens.shape[1] % LANES == 0 and wg.shape[0] % LANES == 0:
        return fused(kv_n, tp_n, *arrays)
    return shards(*arrays)


def solution(mesh):
    placed = (
        P("dp", ("kv", "tp")),
        P(),
        P("kv", "tp"),
        P("dp", "kv", "tp", None),
        P("dp", "kv", "tp", None),
        P("tp"),
        P(),
        P("kv", "tp"),
        P(),
        P(("kv", "tp"), None),
        P(("kv", "tp"), None),
        P(("kv", "tp"), None),
    )
    return jax.shard_map(
        functools.partial(layer, mesh.shape["kv"], mesh.shape["tp"]),
        mesh=mesh, in_specs=placed, out_specs=P("dp", ("kv", "tp")), check_vma=False
    )
```
